512 devices in a mesh: kv: 64 (over z, y), tp: 8 (over x, core).
Axes of the slice: x: 4, y: 4, z: 16, core: 2. Of those that a mesh axis runs over, the one named last changes fastest.
Arguments:
- residual_in: bfloat16 [384, 2048], P('kv', 'tp'), may hold values from -36 to 36
- gain_pre: float32 [2048], P('tp'), may hold values from 0.1 to 1.9
- gate_pre: bfloat16 [2048, 5632], P('tp', 'kv'), may hold values from -0.125 to 0.125
- up_pre: bfloat16 [2048, 5632], P('tp', 'kv'), may hold values from -0.125 to 0.125
- down_pre: bfloat16 [5632, 2048], P('kv', 'tp'), may hold values from -0.078125 to 0.078125
- gain_mix: float32 [2048], replicated, may hold values from 0.1 to 1.9
- query_weight: bfloat16 [2048, 2048], P('kv', 'tp'), may hold values from -0.125 to 0.125
- forget_weight: bfloat16 [2048, 2048], P('kv', 'tp'), may hold values from -0.125 to 0.125
- value_weight: bfloat16 [2048, 2048], P('kv', 'tp'), may hold values from -0.125 to 0.125
- outgate_weight: bfloat16 [2048, 2048], P('kv', 'tp'), may hold values from -0.125 to 0.125
- lower_bound: float32 [2048], P('tp'), may hold values from 0.05 to 0.95
- head_gain: float32 [2048], P('tp'), may hold values from 0.1 to 1.9
- out_weight: bfloat16 [2048, 2048], P('tp'), may hold values from -0.125 to 0.125
- gain_post: float32 [2048], P('tp'), may hold values from 0.1 to 1.9
- gate_post: bfloat16 [2048, 5632], P('tp', 'kv'), may hold values from -0.125 to 0.125
- up_post: bfloat16 [2048, 5632], P('tp', 'kv'), may hold values from -0.125 to 0.125
- down_post: bfloat16 [5632, 2048], P('kv', 'tp'), may hold values from -0.078125 to 0.078125
- memory_state: float32 [384, 16, 128, 128], P('kv', 'tp'), may hold values from -4 to 4
Outputs:
- layer_out: bfloat16 [384, 2048], P('kv', 'tp')
- next_state: float32 [384, 16, 128, 128], P('kv', 'tp')
The draws below stay inside these ranges and needn't reach their ends.
All inputs are finite; a program needn't handle non-finite values.
Results may differ from the reference program's by a relative error of at most 0.014.
Values may be sent and summed in bfloat16 or wider, within the bound.
No kernel may reach another device: no remote copies, remote signals or barrier semaphores. Data moves between devices by JAX's collectives and lax.ppermute only.
A program may use at most 64 MiB of HBM per device.

```python
import math
import jax
import jax.numpy as jnp
from jax import lax

D = 2048
FF = 5632
HEADS = 16
HEAD_DIM = 128
HW = 2048
BATCH = 384


def draw_residual_in(key, part):
    key_base = jax.random.fold_in(key, 11)
    key_cols = jax.random.fold_in(key, 12)
    key_rows = jax.random.fold_in(key, 13)
    column_pos = jnp.arange(D, dtype=jnp.float32) / D
    col_scale = 4.0 ** column_pos * jax.random.uniform(key_cols, (D,), jnp.float32, 0.5, 1.5)
    row_scale = jnp.exp(jax.random.uniform(key_rows, (BATCH, 1), jnp.float32, 0.0, math.log(10.0)))
    base_vals = jnp.clip(jax.random.normal(key_base, (BATCH, D), jnp.float32), -4.0, 4.0)
    return (0.15 * base_vals * col_scale[None, :] * row_scale).astype(jnp.bfloat16)


def block_scale(key, dims, split, smallest, high):
    factor_of = 1.0
    for dim, shards_of in split:
        heights = jax.random.uniform(jax.random.fold_in(jax.random.fold_in(key, 6), dim), (shards_of,), jnp.float32, smallest / len(split), high / len(split))
        factor_of = factor_of * jnp.repeat(jnp.exp(heights), dims[dim] // shards_of).reshape((-1,) + (1,) * (len(dims) - 1 - dim))
    return factor_of


def bell_draw(rng, extent, scale, reach, cuts=(), kind=jnp.bfloat16):
    array = scale * jax.random.normal(rng, extent, jnp.float32)
    if cuts:
        array = array * block_scale(rng, extent, cuts, -0.22, 0.18)
    return jnp.clip(array, -reach, reach).astype(kind)


def setup_inputs(seed: int = 0) -> dict:
    key_of = jax.random.split(jax.random.key(seed), 19)
    residual_in = draw_residual_in(jax.random.fold_in(key_of[18], 71), 0)
    gain_pre = jnp.clip(1.0 + 0.18 * jax.random.normal(key_of[1], (D,), jnp.float32), 0.1, 1.9)
    gate_pre = bell_draw(key_of[2], (D, FF), D ** -0.5, 0.125, ((0, 8), (1, 64)))
    up_pre = bell_draw(key_of[3], (D, FF), D ** -0.5, 0.125, ((0, 8), (1, 64)))
    down_pre = bell_draw(key_of[4], (FF, D), FF ** -0.5, 0.078125, ((0, 64), (1, 8)))
    gain_mix = jnp.clip(1.0 + 0.18 * jax.random.normal(key_of[5], (D,), jnp.float32), 0.1, 1.9)
    query_weight = bell_draw(key_of[6], (D, HW), D ** -0.5, 0.125, ((0, 64), (1, 8)))
    forget_weight = bell_draw(key_of[7], (D, HW), D ** -0.5, 0.125, ((0, 64), (1, 8)))
    value_weight = bell_draw(key_of[8], (D, HW), D ** -0.5, 0.125, ((0, 64), (1, 8)))
    outgate_weight = bell_draw(key_of[9], (D, HW), D ** -0.5, 0.125, ((0, 64), (1, 8)))
    lower_bound = jnp.clip(0.05 + 0.9 * jax.random.uniform(key_of[10], (HW,), jnp.float32) ** block_scale(key_of[10], (HW,), ((0, 8),), -0.2, 0.2), 0.05, 0.95)
    head_gain = jnp.clip(1.0 + 0.18 * jax.random.normal(key_of[11], (HW,), jnp.float32), 0.1, 1.9)
    out_weight = bell_draw(key_of[12], (HW, D), HW ** -0.5, 0.125, ((0, 8),))
    gain_post = jnp.clip(1.0 + 0.18 * jax.random.normal(key_of[13], (D,), jnp.float32), 0.1, 1.9)
    gate_post = bell_draw(key_of[14], (D, FF), D ** -0.5, 0.125, ((0, 8), (1, 64)))
    up_post = bell_draw(key_of[15], (D, FF), D ** -0.5, 0.125, ((0, 8), (1, 64)))
    down_post = bell_draw(key_of[16], (FF, D), FF ** -0.5, 0.078125, ((0, 64), (1, 8)))
    memory_state = bell_draw(key_of[17], (BATCH, HEADS, HEAD_DIM, HEAD_DIM), 0.5, 4.0, ((0, 64), (1, 8)), jnp.float32)
    return dict(residual_in=residual_in, gain_pre=gain_pre, gate_pre=gate_pre, up_pre=up_pre, down_pre=down_pre, gain_mix=gain_mix, query_weight=query_weight, forget_weight=forget_weight, value_weight=value_weight, outgate_weight=outgate_weight, lower_bound=lower_bound, head_gain=head_gain, out_weight=out_weight, gain_post=gain_post, gate_post=gate_post, up_post=up_post, down_post=down_post, memory_state=memory_state)


EPSILON = 1e-06

def channel_mixer(stream, gain_vec, gate_weight, up_weight, down_weight):
    widened = stream.astype(jnp.float32)
    inverse = lax.rsqrt(lax.optimization_barrier(jnp.mean(widened * widened, axis=1, keepdims=True)) + EPSILON)
    scaled = (widened * gain_vec).astype(jnp.bfloat16)
    gate_sum = jnp.dot(scaled, gate_weight, preferred_element_type=jnp.float32) * inverse
    up_sum = jnp.dot(scaled, up_weight, preferred_element_type=jnp.float32) * inverse
    hidden = (jax.nn.silu(gate_sum) * up_sum).astype(jnp.bfloat16)
    return jnp.dot(hidden, down_weight, preferred_element_type=jnp.float32)

def token_mixer(stream, gain_mix, query_weight, forget_weight, value_weight, outgate_weight, lower_bound, head_gain, out_weight, memory_state):
    widened = stream.astype(jnp.float32)
    inverse = lax.rsqrt(lax.optimization_barrier(jnp.mean(widened * widened, axis=1, keepdims=True)) + EPSILON)
    scaled = (widened * gain_mix).astype(jnp.bfloat16)
    batch_rows = stream.shape[0]

    def project(weight_mat):
        product = jnp.dot(scaled, weight_mat, preferred_element_type=jnp.float32) * inverse
        return product.reshape(batch_rows, HEADS, HEAD_DIM)
    query_pre = project(query_weight)
    forget_pre = project(forget_weight)
    value_pre = project(value_weight)
    outgate_pre = project(outgate_weight)
    floor_rate = lower_bound.reshape(HEADS, HEAD_DIM)
    log_keep = jnp.logaddexp(jnp.log(floor_rate), jnp.log1p(-floor_rate) + jax.nn.log_sigmoid(forget_pre))
    inject = (1.0 - floor_rate) * jax.nn.sigmoid(-forget_pre)
    next_state = jnp.exp(log_keep)[..., None] * memory_state + inject[..., None] * value_pre[:, :, None, :]
    readout = jnp.einsum('bhk,bhkv->bhv', jax.nn.silu(query_pre), next_state, precision=lax.Precision.HIGHEST)
    normed = readout * lax.rsqrt(lax.optimization_barrier(jnp.mean(readout * readout, axis=2, keepdims=True)) + EPSILON) * head_gain.reshape(HEADS, HEAD_DIM)
    mixed_heads = (normed * jax.nn.silu(outgate_pre)).reshape(batch_rows, HEADS * HEAD_DIM).astype(jnp.bfloat16)
    mixed = jnp.dot(mixed_heads, out_weight, preferred_element_type=jnp.float32)
    return (mixed, next_state)

def reference(residual_in, gain_pre, gate_pre, up_pre, down_pre, gain_mix, query_weight, forget_weight, value_weight, outgate_weight, lower_bound, head_gain, out_weight, gain_post, gate_post, up_post, down_post, memory_state):
    branch_a = channel_mixer(residual_in, gain_pre, gate_pre, up_pre, down_pre)
    stream_a = (residual_in.astype(jnp.float32) + 0.5 * branch_a).astype(jnp.bfloat16)
    mixed, next_state = token_mixer(stream_a, gain_mix, query_weight, forget_weight, value_weight, outgate_weight, lower_bound, head_gain, out_weight, memory_state)
    stream_b = (stream_a.astype(jnp.float32) + mixed).astype(jnp.bfloat16)
    branch_b = channel_mixer(stream_b, gain_post, gate_post, up_post, down_post)
    layer_out = (stream_b.astype(jnp.float32) + 0.5 * branch_b).astype(jnp.bfloat16)
    return (layer_out, next_state)
```

```python
import jax
import jax.numpy as jnp
from jax import lax
from jax.sharding import Mesh, PartitionSpec as P

D = 2048
HEAD_DIM = 128
EPSILON = 1e-06
TP = ("x", "c")

f32 = jnp.float32
bf16 = jnp.bfloat16


def exchanged(tiles, axis):
    return lax.all_to_all(tiles, axis, split_axis=0, concat_axis=0, tiled=True)


def gathered(array, axis):
    return exchanged(jnp.broadcast_to(array, (lax.axis_size(axis), *array.shape)), axis)


def dot(a, b, da, db):
    return lax.dot_general(a, b, (((da,), (db,)), ((), ())), preferred_element_type=f32)


def padded(array, rows):
    return jnp.pad(array, ((0, rows - array.shape[0]), (0, 0)))


def hidden_units(rows, gain_vec, gate_t, up_t, extra):
    tp = lax.axis_size(TP)
    n = rows.shape[0]
    widened = rows.astype(f32)
    squares = jnp.sum(widened * widened, axis=1)
    scaled = (widened * gain_vec).astype(bf16)
    gate_part = dot(gate_t, scaled, 1, 1).astype(bf16)
    up_part = dot(up_t, scaled, 1, 1).astype(bf16)
    unit = gate_part.shape[0] // tp
    tiles = [
        gate_part.reshape(tp, unit, n),
        up_part.reshape(tp, unit, n),
        jnp.broadcast_to(squares.astype(bf16), (tp, 8, n)),
    ]
    if extra is not None:
        tiles.append(extra)
    arrived = exchanged(jnp.concatenate(tiles, axis=1), TP)
    summed = arrived[:, : 2 * unit + 8].astype(f32).sum(axis=0)
    inverse = lax.rsqrt(summed[2 * unit] / D + EPSILON)[None, :]
    hidden = (jax.nn.silu(summed[:unit] * inverse) * (summed[unit : 2 * unit] * inverse)).astype(bf16)
    every = gathered(hidden, TP).reshape(tp * unit, n)
    return every, arrived[:, 2 * unit + 8 :]


def shards(
    residual_in,
    gain_pre,
    gate_pre,
    up_pre,
    down_pre,
    gain_mix,
    query_weight,
    forget_weight,
    value_weight,
    outgate_weight,
    lower_bound,
    head_gain,
    out_weight,
    gain_post,
    gate_post,
    up_post,
    down_post,
    memory_state,
):
    nz, ny, tp = lax.axis_size("z"), lax.axis_size("y"), lax.axis_size(TP)
    z_at, t_at = lax.axis_index("z"), lax.axis_index(TP)
    own, width = residual_in.shape
    rows = nz * own
    units = gate_pre.shape[1]
    unit = -(-units * ny // (8 * tp)) * 8 * tp // ny
    block = width * tp // nz
    piece = block // tp
    halves = width // block

    first = jnp.concatenate([padded(gate_pre.T, unit), padded(up_pre.T, unit)], axis=0)
    first = gathered(first, "y")
    gate_pre_t = first[:, :unit].reshape(ny * unit, width)
    up_pre_t = first[:, unit:].reshape(ny * unit, width)

    down_t = down_pre.T.reshape(halves, tp, piece, units).swapaxes(0, 1)
    down_t = exchanged(down_t.reshape(tp, halves * piece, units), TP).reshape(width, units)
    kept = query_weight.shape[0]
    second = jnp.concatenate(
        [
            padded(down_t.T, unit),
            padded(gate_post.T, unit),
            padded(up_post.T, unit),
            padded(down_post, unit),
            query_weight,
            forget_weight,
            value_weight,
            outgate_weight,
        ],
        axis=0,
    )
    second = gathered(second, "y")
    down_pre_all, gate_post_t, up_post_t, down_post_all = (
        second[:, k * unit : (k + 1) * unit].reshape(ny * unit, width) for k in range(4)
    )
    mixers = [
        second[:, 4 * unit + k * kept : 4 * unit + (k + 1) * kept].reshape(ny * kept, width)
        for k in range(4)
    ]

    all_rows = gathered(residual_in, "z").reshape(rows, width)
    turned = all_rows.T.reshape(halves, tp, piece, rows).swapaxes(0, 1)
    hidden, residual = hidden_units(
        all_rows, gain_pre, gate_pre_t, up_pre_t, turned.reshape(tp, halves * piece, rows)
    )
    residual = lax.dynamic_index_in_dim(
        residual.reshape(nz, piece, rows), z_at, axis=0, keepdims=False
    )
    part = dot(down_pre_all, hidden, 0, 0).astype(bf16)
    branch = exchanged(part.reshape(nz, piece, rows), "z").astype(f32).sum(axis=0)
    stream_piece = (residual.astype(f32) + 0.5 * branch).astype(bf16)

    stream_t = gathered(stream_piece, TP).reshape(block, rows)
    widened = stream_t.astype(f32)
    squares = jnp.sum(widened * widened, axis=0)
    gain_block = lax.dynamic_slice_in_dim(gain_mix, z_at * block, block)
    scaled = (widened * gain_block[:, None]).astype(bf16)
    parts = [dot(scaled, weight, 0, 0).astype(bf16).reshape(nz, own, width) for weight in mixers]
    mine = z_at // halves == t_at
    note = jnp.where(
        mine,
        stream_t.T.reshape(nz, own, block),
        jnp.broadcast_to(squares.astype(bf16).reshape(nz, own, 1), (nz, own, block)),
    )
    arrived = exchanged(jnp.concatenate([*parts, note], axis=2), "z")
    projected = arrived[:, :, : 4 * width].astype(f32).sum(axis=0)
    notes = arrived[:, :, 4 * width :]
    stream_a = lax.dynamic_slice_in_dim(notes, t_at * halves, halves, axis=0)
    stream_a = stream_a.swapaxes(0, 1).reshape(own, width).astype(f32)
    elsewhere = (jnp.arange(nz) // halves != t_at)[:, None]
    total = jnp.sum(jnp.where(elsewhere, notes[:, :, 0].astype(f32), 0.0), axis=0)
    total = total + jnp.sum(stream_a * stream_a, axis=1)
    projected = projected * lax.rsqrt(total / D + EPSILON)[:, None]

    heads = width // HEAD_DIM
    query_pre, forget_pre, value_pre, outgate_pre = (
        projected[:, k * width : (k + 1) * width].reshape(own, heads, HEAD_DIM) for k in range(4)
    )
    floor_rate = lower_bound.reshape(heads, HEAD_DIM)
    log_keep = jnp.logaddexp(
        jnp.log(floor_rate), jnp.log1p(-floor_rate) + jax.nn.log_sigmoid(forget_pre)
    )
    inject = (1.0 - floor_rate) * jax.nn.sigmoid(-forget_pre)
    next_state = (
        jnp.exp(log_keep)[..., None] * memory_state + inject[..., None] * value_pre[:, :, None, :]
    )
    readout = jnp.einsum(
        "bhk,bhkv->bhv", jax.nn.silu(query_pre), next_state, precision=lax.Precision.HIGHEST
    )
    normed = (
        readout
        * lax.rsqrt(jnp.mean(readout * readout, axis=2, keepdims=True) + EPSILON)
        * head_gain.reshape(heads, HEAD_DIM)
    )
    mixed_heads = (normed * jax.nn.silu(outgate_pre)).reshape(own, width).astype(bf16)
    partial_out = dot(mixed_heads, out_weight, 1, 0).astype(bf16)
    mixed = exchanged(partial_out.reshape(own, tp, width).swapaxes(0, 1), TP)
    stream_b = (stream_a + mixed.astype(f32).sum(axis=0)).astype(bf16)

    all_rows = gathered(stream_b, "z").reshape(rows, width)
    hidden, _ = hidden_units(all_rows, gain_post, gate_post_t, up_post_t, None)
    part = dot(hidden, down_post_all, 0, 0).astype(bf16)
    branch = exchanged(part.reshape(nz, own, width), "z").astype(f32).sum(axis=0)
    layer_out = (stream_b.astype(f32) + 0.5 * branch).astype(bf16)
    return (layer_out, next_state)


def solution(mesh):
    grid = Mesh(mesh.devices.reshape(16, 4, 4, 2), ("z", "y", "x", "c"))
    kv = ("z", "y")
    in_specs = (
        P(kv, TP),
        P(TP),
        P(TP, kv),
        P(TP, kv),
        P(kv, TP),
        P(),
        P(kv, TP),
        P(kv, TP),
        P(kv, TP),
        P(kv, TP),
        P(TP),
        P(TP),
        P(TP, None),
        P(TP),
        P(TP, kv),
        P(TP, kv),
        P(kv, TP),
        P(kv, TP, None, None),
    )
    out_specs = (P(kv, TP), P(kv, TP, None, None))
    return jax.shard_map(shards, mesh=grid, in_specs=in_specs, out_specs=out_specs, check_vma=False)
```

```python
import jax
import jax.numpy as jnp
from jax import lax
from jax.sharding import Mesh, PartitionSpec as P

D = 2048
HEAD_DIM = 128
EPSILON = 1e-06
TP = ("x", "c")

f32 = jnp.float32
bf16 = jnp.bfloat16


def exchanged(tiles, axis):
    return lax.all_to_all(tiles, axis, split_axis=0, concat_axis=0, tiled=True)


def gathered(array, axis):
    return exchanged(jnp.broadcast_to(array, (lax.axis_size(axis), *array.shape)), axis)


def dot(a, b, da, db):
    return lax.dot_general(a, b, (((da,), (db,)), ((), ())), preferred_element_type=f32)


def from_others(array, axis):
    n = lax.axis_size(axis)
    later = [
        lax.ppermute(array, axis, [(i, (i - k) % n) for i in range(n)]) for k in range(1, n)
    ]
    return [array, *later]


def rolled(array, shift):
    return lax.dynamic_slice_in_dim(
        jnp.concatenate([array, array], axis=0), shift, array.shape[0], axis=0
    )


def padded(array, rows):
    return jnp.pad(array, ((0, rows - array.shape[0]), (0, 0)))


def hidden_units(rows, gain_vec, gate_t, up_t, extra):
    tp = lax.axis_size(TP)
    n = rows.shape[0]
    widened = rows.astype(f32)
    squares = jnp.sum(widened * widened, axis=1)
    scaled = (widened * gain_vec).astype(bf16)
    gate_part = dot(gate_t, scaled, 1, 1).astype(bf16)
    up_part = dot(up_t, scaled, 1, 1).astype(bf16)
    unit = gate_part.shape[0] // tp
    tiles = [
        gate_part.reshape(tp, unit, n),
        up_part.reshape(tp, unit, n),
        jnp.broadcast_to(squares.astype(bf16), (tp, 8, n)),
        *extra,
    ]
    arrived = exchanged(jnp.concatenate(tiles, axis=1), TP)
    summed = arrived[:, : 2 * unit + 8].astype(f32).sum(axis=0)
    inverse = lax.rsqrt(summed[2 * unit] / D + EPSILON)[None, :]
    hidden = (jax.nn.silu(summed[:unit] * inverse) * (summed[unit : 2 * unit] * inverse)).astype(bf16)
    every = gathered(hidden, TP).reshape(tp * unit, n)
    return every, arrived[:, 2 * unit + 8 :]


def shards(
    residual_in,
    gain_pre,
    gate_pre,
    up_pre,
    down_pre,
    gain_mix,
    query_weight,
    forget_weight,
    value_weight,
    outgate_weight,
    lower_bound,
    head_gain,
    out_weight,
    gain_post,
    gate_post,
    up_post,
    down_post,
    memory_state,
):
    nz, ny, tp = lax.axis_size("z"), lax.axis_size("y"), lax.axis_size(TP)
    z_at, t_at = lax.axis_index("z"), lax.axis_index(TP)
    own, width = residual_in.shape
    rows = nz * own
    units = gate_pre.shape[1]
    unit = -(-units * ny // (8 * tp)) * 8 * tp // ny
    block = width * tp // nz
    piece = block // tp
    halves = width // block
    kept = query_weight.shape[0]

    all_rows = gathered(residual_in, "z")
    first = jnp.concatenate(
        [padded(gate_pre.T, unit), padded(up_pre.T, unit), padded(down_pre, unit)], axis=0
    )
    first = from_others(first, "y")
    first = jnp.stack(first)
    second = jnp.concatenate(
        [
            padded(gate_post.T, unit),
            padded(up_post.T, unit),
            padded(down_post, unit),
            query_weight,
            forget_weight,
            value_weight,
            outgate_weight,
        ],
        axis=0,
    )
    gain_block = lax.dynamic_slice_in_dim(gain_mix, z_at * block, block)
    gain_block = rolled(gain_block, kept * lax.axis_index("y"))
    small = jnp.stack([gain_post, head_gain, lower_bound])
    down_tiles = first[:, 2 * unit :].swapaxes(1, 2).reshape(ny, halves, tp, piece, unit)
    down_tiles = down_tiles.transpose(2, 0, 1, 3, 4).reshape(tp, ny * halves * piece, unit)
    all_rows, first, second, gain_block, small, down_tiles = lax.optimization_barrier(
        (all_rows, first, second, gain_block, small, down_tiles)
    )
    gate_pre_t = first[:, :unit].reshape(ny * unit, width)
    up_pre_t = first[:, unit : 2 * unit].reshape(ny * unit, width)

    all_rows = all_rows.reshape(rows, width)
    turned = all_rows.T.reshape(halves, tp, piece, rows).swapaxes(0, 1)
    hidden, extra = hidden_units(
        all_rows,
        gain_pre,
        gate_pre_t,
        up_pre_t,
        (turned.reshape(tp, halves * piece, rows), down_tiles),
    )
    residual = lax.dynamic_index_in_dim(
        extra[:, : halves * piece].reshape(nz, piece, rows), z_at, axis=0, keepdims=False
    )
    down_pre_t = extra[:, halves * piece :].reshape(tp, ny, halves * piece, unit)
    part = sum(
        dot(
            down_pre_t[:, k].reshape(width, unit),
            hidden[k * unit : (k + 1) * unit],
            1,
            0,
        )
        for k in range(ny)
    ).astype(bf16)
    second = jnp.stack(from_others(second, "y"))
    branch = exchanged(part.reshape(nz, piece, rows), "z")
    branch = branch.astype(f32).sum(axis=0)
    stream_piece = (residual.astype(f32) + 0.5 * branch).astype(bf16)

    gate_post_t, up_post_t, down_post_all = (
        second[:, k * unit : (k + 1) * unit].reshape(ny * unit, width) for k in range(3)
    )
    mixers = jnp.concatenate(
        [
            second[:, 3 * unit + k * kept : 3 * unit + (k + 1) * kept].reshape(ny * kept, width)
            for k in range(4)
        ],
        axis=1,
    )
    stream_piece, gate_post_t, up_post_t, down_post_all, mixers = lax.optimization_barrier(
        (stream_piece, gate_post_t, up_post_t, down_post_all, mixers)
    )
    stream_t = gathered(stream_piece, TP).reshape(block, rows)
    widened = stream_t.astype(f32)
    squares = jnp.sum(widened * widened, axis=0)
    scaled = rolled(widened, kept * lax.axis_index("y"))
    scaled = (scaled * gain_block[:, None]).astype(bf16)
    heads = width // HEAD_DIM
    parts = dot(scaled, mixers, 0, 0).astype(bf16)
    parts = parts.reshape(nz, own, 4 * heads, HEAD_DIM).swapaxes(1, 2)
    mine = z_at // halves == t_at
    note = jnp.where(
        mine,
        stream_t.T.reshape(nz, own, block),
        jnp.broadcast_to(squares.astype(bf16).reshape(nz, own, 1), (nz, own, block)),
    )
    message = jnp.concatenate([parts.reshape(nz, 4 * heads * own, HEAD_DIM), note], axis=1)
    arrived = exchanged(message, "z")
    projected = arrived[:, : 4 * heads * own].astype(f32).sum(axis=0)
    notes = arrived[:, 4 * heads * own :]
    stream_a = lax.dynamic_slice_in_dim(notes, t_at * halves, halves, axis=0)
    stream_a = stream_a.swapaxes(0, 1).reshape(own, width).astype(f32)
    elsewhere = (jnp.arange(nz) // halves != t_at)[:, None]
    total = jnp.sum(jnp.where(elsewhere, notes[:, :, 0].astype(f32), 0.0), axis=0)
    total = total + jnp.sum(stream_a * stream_a, axis=1)
    projected = projected.reshape(4, heads, own, HEAD_DIM)
    projected = projected * lax.rsqrt(total / D + EPSILON)[:, None]

    query_pre, forget_pre, value_pre, outgate_pre = (
        projected[k].swapaxes(0, 1) for k in range(4)
    )
    floor_rate = small[2].reshape(heads, HEAD_DIM)
    log_keep = jnp.logaddexp(
        jnp.log(floor_rate), jnp.log1p(-floor_rate) + jax.nn.log_sigmoid(forget_pre)
    )
    inject = (1.0 - floor_rate) * jax.nn.sigmoid(-forget_pre)
    next_state = (
        jnp.exp(log_keep)[..., None] * memory_state + inject[..., None] * value_pre[:, :, None, :]
    )
    readout = jnp.einsum(
        "bhk,bhkv->bhv", jax.nn.silu(query_pre), next_state, precision=lax.Precision.HIGHEST
    )
    normed = (
        readout
        * lax.rsqrt(jnp.mean(readout * readout, axis=2, keepdims=True) + EPSILON)
        * small[1].reshape(heads, HEAD_DIM)
    )
    mixed_heads = (normed * jax.nn.silu(outgate_pre)).reshape(own, width).astype(bf16)
    partial_out = dot(mixed_heads, out_weight, 1, 0).astype(bf16)
    mixed = exchanged(partial_out.reshape(own, tp, width).swapaxes(0, 1), TP)
    stream_b = (stream_a + mixed.astype(f32).sum(axis=0)).astype(bf16)

    all_rows = gathered(stream_b, "z").reshape(rows, width)
    hidden, _ = hidden_units(all_rows, small[0], gate_post_t, up_post_t, ())
    part = dot(hidden, down_post_all, 0, 0).astype(bf16)
    branch = exchanged(part.reshape(nz, own, width), "z").astype(f32).sum(axis=0)
    layer_out = (stream_b.astype(f32) + 0.5 * branch).astype(bf16)
    return (layer_out, next_state)


def solution(mesh):
    grid = Mesh(mesh.devices.reshape(16, 4, 4, 2), ("z", "y", "x", "c"))
    kv = ("z", "y")
    in_specs = (
        P(kv, TP),
        P(TP),
        P(TP, kv),
        P(TP, kv),
        P(kv, TP),
        P(),
        P(kv, TP),
        P(kv, TP),
        P(kv, TP),
        P(kv, TP),
        P(TP),
        P(TP),
        P(TP, None),
        P(TP),
        P(TP, kv),
        P(TP, kv),
        P(kv, TP),
        P(kv, TP, None, None),
    )
    out_specs = (P(kv, TP), P(kv, TP, None, None))

    return jax.shard_map(shards, mesh=grid, in_specs=in_specs, out_specs=out_specs, check_vma=False)
```

```python
import jax
import jax.numpy as jnp
from jax import lax
from jax.experimental import pallas as pl
from jax.experimental.pallas import tpu as pltpu
from jax.sharding import Mesh, PartitionSpec as P

D = 2048
HEAD_DIM = 128
EPSILON = 1e-06
TP = ("x", "c")

f32 = jnp.float32
bf16 = jnp.bfloat16


def exchanged(tiles, axis):
    return lax.all_to_all(tiles, axis, split_axis=0, concat_axis=0, tiled=True)


def gathered(array, axis):
    return exchanged(jnp.broadcast_to(array, (lax.axis_size(axis), *array.shape)), axis)


def dot(a, b, da, db):
    return lax.dot_general(a, b, (((da,), (db,)), ((), ())), preferred_element_type=f32)


def from_others(array, axis):
    n = lax.axis_size(axis)
    later = [
        lax.ppermute(array, axis, [(i, (i - k) % n) for i in range(n)]) for k in range(1, n)
    ]
    return [array, *later]


def staged(unit, copies, ups, downs, kept, small):
    rows, gate_a, up_a, down_a, gate_b, up_b, down_b, *projections = ups + downs + kept
    units, width = gate_a.shape
    height = projections[0].shape[0]
    n_in = 7 + len(projections) + len(small)

    def kernel(*refs):
        ins, outs = refs[:n_in], refs[n_in : n_in + 3 + len(small)]
        held, sems = refs[-2], refs[-1]
        spread, first, second = outs[:3]
        moves = [(ins[0], held)]
        moves += [(ins[1 + k], first.at[pl.ds(k * unit, units)]) for k in range(3)]
        moves += [(ins[4 + k], second.at[pl.ds(k * unit, units)]) for k in range(3)]
        for k in range(len(projections)):
            moves.append((ins[7 + k], second.at[pl.ds(3 * unit + k * height, height)]))
        for k in range(len(small)):
            moves.append((ins[7 + len(projections) + k], outs[3 + k]))
        started = [pltpu.make_async_copy(a, b, sems.at[k]) for k, (a, b) in enumerate(moves)]
        for move in started:
            move.start()
        if unit > units:
            blank = jnp.zeros((unit - units, width), first.dtype)
            for k in range(3):
                first[pl.ds(k * unit + units, unit - units), :] = blank
                second[pl.ds(k * unit + units, unit - units), :] = blank
        started[0].wait()
        for k in range(copies):
            spread[k] = held[...]
        for move in started[1:]:
            move.wait()

    arrays = [rows, gate_a, up_a, down_a, gate_b, up_b, down_b, *projections, *small]
    vmem = pl.BlockSpec(memory_space=pltpu.VMEM)
    shapes = [
        jax.ShapeDtypeStruct((copies, *rows.shape), bf16),
        jax.ShapeDtypeStruct((3 * unit, width), bf16),
        jax.ShapeDtypeStruct((3 * unit + len(projections) * height, width), bf16),
        *[jax.ShapeDtypeStruct(v.shape, v.dtype) for v in small],
    ]
    return pl.pallas_call(
        kernel,
        out_shape=shapes,
        in_specs=[pl.BlockSpec(memory_space=pl.ANY)] * n_in,
        out_specs=[vmem] * len(shapes),
        scratch_shapes=[pltpu.VMEM(rows.shape, bf16), pltpu.SemaphoreType.DMA((n_in,))],
    )(*arrays)


def doubled(array, axis, apart):
    n = lax.axis_size(axis)
    return jnp.concatenate([array, lax.ppermute(array, axis, [(i, i ^ apart) for i in range(n)])])


def reordered(blocks, at):
    blocks = jnp.stack([blocks[0], blocks[2], blocks[1], blocks[3]])
    halves = jnp.concatenate([blocks[2:], blocks[:2]])
    blocks = jnp.where(at % 2 == 1, halves, blocks)
    pairs = jnp.concatenate([blocks[1:2], blocks[0:1], blocks[3:4], blocks[2:3]])
    return jnp.where(at // 2 == 1, pairs, blocks)


def hidden_units(rows, gain_vec, gate_t, up_t, extra):
    tp = lax.axis_size(TP)
    n = rows.shape[0]
    widened = rows.astype(f32)
    squares = jnp.sum(widened * widened, axis=1)
    scaled = (widened * gain_vec).astype(bf16)
    gate_part = dot(gate_t, scaled, 1, 1).astype(bf16)
    up_part = dot(up_t, scaled, 1, 1).astype(bf16)
    unit = gate_part.shape[0] // tp
    tiles = [
        gate_part.reshape(tp, unit, n),
        up_part.reshape(tp, unit, n),
        jnp.broadcast_to(squares.astype(bf16), (tp, 8, n)),
        *extra,
    ]
    arrived = exchanged(jnp.concatenate(tiles, axis=1), TP)
    summed = arrived[:, : 2 * unit + 8].astype(f32).sum(axis=0)
    inverse = lax.rsqrt(summed[2 * unit] / D + EPSILON)[None, :]
    hidden = (jax.nn.silu(summed[:unit] * inverse) * (summed[unit : 2 * unit] * inverse)).astype(bf16)
    every = gathered(hidden, TP).reshape(tp * unit, n)
    return every, arrived[:, 2 * unit + 8 :]


def shards(
    residual_in,
    gain_pre,
    gate_pre,
    up_pre,
    down_pre,
    gain_mix,
    query_weight,
    forget_weight,
    value_weight,
    outgate_weight,
    lower_bound,
    head_gain,
    out_weight,
    gain_post,
    gate_post,
    up_post,
    down_post,
    memory_state,
):
    nz, ny, tp = lax.axis_size("z"), lax.axis_size("y"), lax.axis_size(TP)
    z_at, t_at = lax.axis_index("z"), lax.axis_index(TP)
    own, width = residual_in.shape
    rows = nz * own
    units = gate_pre.shape[1]
    unit = -(-units * ny // (8 * tp)) * 8 * tp // ny
    block = width * tp // nz
    piece = block // tp
    halves = width // block
    kept = query_weight.shape[0]

    y_at = lax.axis_index("y")
    spread, first, second, gain_pre, gain_post, head_gain, lower_bound, gain_mix = staged(
        unit,
        nz,
        [residual_in, gate_pre.T, up_pre.T],
        [down_pre, gate_post.T, up_post.T, down_post],
        [query_weight, forget_weight, value_weight, outgate_weight],
        [v.reshape(-1, HEAD_DIM) for v in (gain_pre, gain_post, head_gain, lower_bound, gain_mix)],
    )
    gain_pre, gain_post = gain_pre.reshape(width), gain_post.reshape(width)
    gain_block = lax.dynamic_slice_in_dim(gain_mix, z_at * block // HEAD_DIM, block // HEAD_DIM)
    gain_block = reordered(gain_block.reshape(ny, kept), y_at).reshape(block)
    first = from_others(first, "y")
    all_rows = exchanged(spread, "z")
    first = jnp.stack(first)
    down_tiles = first[:, 2 * unit :].swapaxes(1, 2).reshape(ny, halves, tp, piece, unit)
    down_tiles = down_tiles.transpose(2, 0, 1, 3, 4).reshape(tp, ny * halves * piece, unit)
    all_rows, first, gain_block, down_tiles = lax.optimization_barrier(
        (all_rows, first, gain_block, down_tiles)
    )
    gate_pre_t = first[:, :unit].reshape(ny * unit, width)
    up_pre_t = first[:, unit : 2 * unit].reshape(ny * unit, width)

    all_rows = all_rows.reshape(rows, width)
    turned = all_rows.T.reshape(halves, tp, piece, rows).swapaxes(0, 1)
    hidden, extra = hidden_units(
        all_rows,
        gain_pre,
        gate_pre_t,
        up_pre_t,
        (turned.reshape(tp, halves * piece, rows), down_tiles),
    )
    residual = lax.dynamic_index_in_dim(
        extra[:, : halves * piece].reshape(nz, piece, rows), z_at, axis=0, keepdims=False
    )
    down_pre_t = extra[:, halves * piece :].reshape(tp, ny, halves * piece, unit)
    part = sum(
        dot(
            down_pre_t[:, k].reshape(width, unit),
            hidden[k * unit : (k + 1) * unit],
            1,
            0,
        )
        for k in range(ny)
    ).astype(bf16)
    second = doubled(second, "y", 2)
    second = doubled(second, "y", 1).reshape(ny, -1, width)
    branch = exchanged(part.reshape(nz, piece, rows), "z")
    branch = branch.astype(f32).sum(axis=0)
    stream_piece = (residual.astype(f32) + 0.5 * branch).astype(bf16)

    gate_post_t, up_post_t, down_post_all = (
        second[:, k * unit : (k + 1) * unit].reshape(ny * unit, width) for k in range(3)
    )
    mixers = jnp.concatenate(
        [
            second[:, 3 * unit + k * kept : 3 * unit + (k + 1) * kept].reshape(ny * kept, width)
            for k in range(4)
        ],
        axis=1,
    )
    stream_piece, gate_post_t, up_post_t, down_post_all, mixers = lax.optimization_barrier(
        (stream_piece, gate_post_t, up_post_t, down_post_all, mixers)
    )
    stream_t = gathered(stream_piece, TP).reshape(block, rows)
    widened = stream_t.astype(f32)
    squares = jnp.sum(widened * widened, axis=0)
    scaled = reordered(widened.reshape(ny, kept, rows), y_at).reshape(block, rows)
    scaled = (scaled * gain_block[:, None]).astype(bf16)
    heads = width // HEAD_DIM
    parts = dot(scaled, mixers, 0, 0).astype(bf16)
    parts = parts.reshape(nz, own, 4 * heads, HEAD_DIM).swapaxes(1, 2)
    mine = z_at // halves == t_at
    note = jnp.where(
        mine,
        stream_t.T.reshape(nz, own, block),
        jnp.broadcast_to(squares.astype(bf16).reshape(nz, own, 1), (nz, own, block)),
    )
    message = jnp.concatenate([parts.reshape(nz, 4 * heads * own, HEAD_DIM), note], axis=1)
    arrived = exchanged(message, "z")
    projected = arrived[:, : 4 * heads * own].astype(f32).sum(axis=0)
    notes = arrived[:, 4 * heads * own :]
    stream_a = lax.dynamic_slice_in_dim(notes, t_at * halves, halves, axis=0)
    stream_a = stream_a.swapaxes(0, 1).reshape(own, width).astype(f32)
    elsewhere = (jnp.arange(nz) // halves != t_at)[:, None]
    total = jnp.sum(jnp.where(elsewhere, notes[:, :, 0].astype(f32), 0.0), axis=0)
    total = total + jnp.sum(stream_a * stream_a, axis=1)
    projected = projected.reshape(4, heads, own, HEAD_DIM)
    projected = projected * lax.rsqrt(total / D + EPSILON)[:, None]

    query_pre, forget_pre, value_pre, outgate_pre = (
        projected[k].swapaxes(0, 1) for k in range(4)
    )
    floor_rate = lower_bound.reshape(heads, HEAD_DIM)
    log_keep = jnp.logaddexp(
        jnp.log(floor_rate), jnp.log1p(-floor_rate) + jax.nn.log_sigmoid(forget_pre)
    )
    inject = (1.0 - floor_rate) * jax.nn.sigmoid(-forget_pre)
    next_state = (
        jnp.exp(log_keep)[..., None] * memory_state + inject[..., None] * value_pre[:, :, None, :]
    )
    readout = jnp.einsum(
        "bhk,bhkv->bhv", jax.nn.silu(query_pre), next_state, precision=lax.Precision.HIGHEST
    )
    normed = (
        readout
        * lax.rsqrt(jnp.mean(readout * readout, axis=2, keepdims=True) + EPSILON)
        * head_gain.reshape(heads, HEAD_DIM)
    )
    mixed_heads = (normed * jax.nn.silu(outgate_pre)).reshape(own, width).astype(bf16)
    partial_out = dot(mixed_heads, out_weight, 1, 0).astype(bf16)
    mixed = exchanged(partial_out.reshape(own, tp, width).swapaxes(0, 1), TP)
    stream_b = (stream_a + mixed.astype(f32).sum(axis=0)).astype(bf16)

    all_rows = gathered(stream_b, "z").reshape(rows, width)
    hidden, _ = hidden_units(all_rows, gain_post, gate_post_t, up_post_t, ())
    part = dot(hidden, down_post_all, 0, 0).astype(bf16)
    branch = exchanged(part.reshape(nz, own, width), "z").astype(f32).sum(axis=0)
    layer_out = (stream_b.astype(f32) + 0.5 * branch).astype(bf16)
    return (layer_out, next_state)


def solution(mesh):
    grid = Mesh(mesh.devices.reshape(16, 4, 4, 2), ("z", "y", "x", "c"))
    kv = ("z", "y")
    in_specs = (
        P(kv, TP),
        P(TP),
        P(TP, kv),
        P(TP, kv),
        P(kv, TP),
        P(),
        P(kv, TP),
        P(kv, TP),
        P(kv, TP),
        P(kv, TP),
        P(TP),
        P(TP),
        P(TP, None),
        P(TP),
        P(TP, kv),
        P(TP, kv),
        P(kv, TP),
        P(kv, TP, None, None),
    )
    out_specs = (P(kv, TP), P(kv, TP, None, None))

    return jax.shard_map(shards, mesh=grid, in_specs=in_specs, out_specs=out_specs, check_vma=False)
```

```python
import jax
import jax.numpy as jnp
from jax import lax
from jax.experimental import pallas as pl
from jax.experimental.pallas import tpu as pltpu
from jax.sharding import Mesh, PartitionSpec as P

D = 2048
HEAD_DIM = 128
EPSILON = 1e-06
TP = ("x", "c")

f32 = jnp.float32
bf16 = jnp.bfloat16


def exchanged(tiles, axis):
    return lax.all_to_all(tiles, axis, split_axis=0, concat_axis=0, tiled=True)


def gathered(array, axis):
    return exchanged(jnp.broadcast_to(array, (lax.axis_size(axis), *array.shape)), axis)


def dot(a, b, da, db):
    return lax.dot_general(a, b, (((da,), (db,)), ((), ())), preferred_element_type=f32)


def from_others(array, axis):
    n = lax.axis_size(axis)
    later = [
        lax.ppermute(array, axis, [(i, (i - k) % n) for i in range(n)]) for k in range(1, n)
    ]
    return [array, *later]


def staged(unit, copies, ups, downs, kept, small):
    rows, gate_a, up_a, down_a, gate_b, up_b, down_b, *projections = ups + downs + kept
    units, width = gate_a.shape
    height = projections[0].shape[0]
    n_in = 7 + len(projections) + len(small)

    def kernel(*refs):
        ins, outs = refs[:n_in], refs[n_in : n_in + 3 + len(small)]
        held, sems = refs[-2], refs[-1]
        spread, first, second = outs[:3]
        moves = [(ins[0], held)]
        moves += [(ins[1 + k], first.at[pl.ds(k * unit, units)]) for k in range(3)]
        moves += [(ins[4 + k], second.at[pl.ds(k * unit, units)]) for k in range(3)]
        for k in range(len(projections)):
            moves.append((ins[7 + k], second.at[pl.ds(3 * unit + k * height, height)]))
        for k in range(len(small)):
            moves.append((ins[7 + len(projections) + k], outs[3 + k]))
        started = [pltpu.make_async_copy(a, b, sems.at[k]) for k, (a, b) in enumerate(moves)]
        for move in started:
            move.start()
        if unit > units:
            blank = jnp.zeros((unit - units, width), first.dtype)
            for k in range(3):
                first[pl.ds(k * unit + units, unit - units), :] = blank
                second[pl.ds(k * unit + units, unit - units), :] = blank
        started[0].wait()
        for k in range(copies):
            spread[k] = held[...]
        for move in started[1:]:
            move.wait()

    arrays = [rows, gate_a, up_a, down_a, gate_b, up_b, down_b, *projections, *small]
    vmem = pl.BlockSpec(memory_space=pltpu.VMEM)
    shapes = [
        jax.ShapeDtypeStruct((copies, *rows.shape), bf16),
        jax.ShapeDtypeStruct((3 * unit, width), bf16),
        jax.ShapeDtypeStruct((3 * unit + len(projections) * height, width), bf16),
        *[jax.ShapeDtypeStruct(v.shape, v.dtype) for v in small],
    ]
    return pl.pallas_call(
        kernel,
        out_shape=shapes,
        in_specs=[pl.BlockSpec(memory_space=pl.ANY)] * n_in,
        out_specs=[vmem] * len(shapes),
        scratch_shapes=[pltpu.VMEM(rows.shape, bf16), pltpu.SemaphoreType.DMA((n_in,))],
    )(*arrays)


def doubled(array, axis, apart):
    n = lax.axis_size(axis)
    return jnp.concatenate([array, lax.ppermute(array, axis, [(i, i ^ apart) for i in range(n)])])


def reordered(blocks, odd, upper):
    blocks = jnp.stack([blocks[0], blocks[2], blocks[1], blocks[3]])
    halves = jnp.concatenate([blocks[2:], blocks[:2]])
    blocks = jnp.where(odd, halves, blocks)
    pairs = jnp.concatenate([blocks[1:2], blocks[0:1], blocks[3:4], blocks[2:3]])
    return jnp.where(upper, pairs, blocks)


def hidden_units(rows, gain_vec, gate_t, up_t, extra, finish, later):
    tp = lax.axis_size(TP)
    n = rows.shape[0]
    widened = rows.astype(f32)
    squares = jnp.sum(widened * widened, axis=1)
    scaled = (widened * gain_vec).astype(bf16)
    gate_part = dot(gate_t, scaled, 1, 1).astype(bf16)
    up_part = dot(up_t, scaled, 1, 1).astype(bf16)
    unit = gate_part.shape[0] // tp
    tiles = [
        gate_part.reshape(tp, unit, n),
        up_part.reshape(tp, unit, n),
        jnp.broadcast_to(squares.astype(bf16), (tp, 8, n)),
        *extra,
    ]
    message, *later = lax.optimization_barrier((jnp.concatenate(tiles, axis=1), *later))
    arrived = exchanged(message, TP)
    summed = arrived[:, : 2 * unit + 8].astype(f32).sum(axis=0)
    inverse = lax.rsqrt(summed[2 * unit] / D + EPSILON)[None, :]
    hidden = (jax.nn.silu(summed[:unit] * inverse) * (summed[unit : 2 * unit] * inverse)).astype(bf16)
    hidden, *rest = lax.optimization_barrier((hidden, *finish(arrived[:, 2 * unit + 8 :]), *later))
    every = gathered(hidden, TP).reshape(tp * unit, n)
    return every, rest


def shards(
    residual_in,
    gain_pre,
    gate_pre,
    up_pre,
    down_pre,
    gain_mix,
    query_weight,
    forget_weight,
    value_weight,
    outgate_weight,
    lower_bound,
    head_gain,
    out_weight,
    gain_post,
    gate_post,
    up_post,
    down_post,
    memory_state,
):
    nz, ny, tp = lax.axis_size("z"), lax.axis_size("y"), lax.axis_size(TP)
    z_at, t_at, y_at = (lax.axis_index(k).astype(jnp.uint32) for k in ("z", TP, "y"))
    own, width = residual_in.shape
    rows = nz * own
    units = gate_pre.shape[1]
    unit = -(-units * ny // (8 * tp)) * 8 * tp // ny
    block = width * tp // nz
    piece = block // tp
    halves = width // block
    kept = query_weight.shape[0]

    spread, first, second, gain_pre, gain_post, head_gain, lower_bound, gain_mix = staged(
        unit,
        nz,
        [residual_in, gate_pre.T, up_pre.T],
        [down_pre, gate_post.T, up_post.T, down_post],
        [query_weight, forget_weight, value_weight, outgate_weight],
        [v.reshape(-1, HEAD_DIM) for v in (gain_pre, gain_post, head_gain, lower_bound, gain_mix)],
    )
    gain_pre, gain_post = gain_pre.reshape(width), gain_post.reshape(width)
    gain_block = lax.dynamic_slice_in_dim(gain_mix, z_at * block // HEAD_DIM, block // HEAD_DIM)
    gain_block = reordered(gain_block.reshape(ny, kept), y_at % 2 == 1, y_at // 2 == 1).reshape(block)
    first = from_others(first, "y")
    second = doubled(second, "y", 2)
    all_rows = exchanged(spread, "z")
    first = jnp.stack(first)
    down_tiles = first[:, 2 * unit :].swapaxes(1, 2).reshape(ny, halves, tp, piece, unit)
    down_tiles = down_tiles.transpose(2, 0, 1, 3, 4).reshape(tp, ny * halves * piece, unit)
    mine = z_at // halves == t_at
    elsewhere = (jnp.arange(nz, dtype=jnp.uint32) // halves != t_at)[:, None]
    note_at = t_at * halves
    odd, upper = y_at % 2 == 1, y_at // 2 == 1
    floor_rate = lower_bound.reshape(-1, HEAD_DIM)
    floors = (jnp.log(floor_rate), jnp.log1p(-floor_rate), 1.0 - floor_rate)
    all_rows, second, first, down_tiles, *known = lax.optimization_barrier(
        (all_rows, second, first, down_tiles, gain_block, gain_pre, gain_post, head_gain)
        + (*floors, mine, elsewhere, note_at, odd, upper, z_at)
    )
    gain_block, gain_pre, gain_post, head_gain, log_floor, log_rest, rest_rate = known[:7]
    mine, elsewhere, note_at, odd, upper, z_at = known[7:]
    others = lax.ppermute(second, "y", [(i, i ^ 1) for i in range(ny)])
    gate_pre_t = first[:, :unit].reshape(ny * unit, width)
    up_pre_t = first[:, unit : 2 * unit].reshape(ny * unit, width)

    all_rows = all_rows.reshape(rows, width)
    turned = all_rows.T.reshape(halves, tp, piece, rows).swapaxes(0, 1)
    own_rows = (tp, halves * piece, rows)

    def finish(extra):
        pieces = extra[:, : halves * piece].reshape(nz, piece, rows)
        return (
            lax.dynamic_index_in_dim(pieces, z_at, axis=0, keepdims=False),
            *[extra[:, k * halves * piece :][:, : halves * piece].reshape(width, unit) for k in range(1, ny + 1)],
        )

    hidden, (residual, *down_pre_t, second, gain_block) = hidden_units(
        all_rows,
        gain_pre,
        gate_pre_t,
        up_pre_t,
        (turned.reshape(own_rows), down_tiles),
        finish,
        (second, gain_block),
    )
    part = sum(
        dot(down_pre_t[k], hidden[k * unit : (k + 1) * unit], 1, 0) for k in range(ny)
    ).astype(bf16)
    second = jnp.concatenate([second, others]).reshape(ny, -1, width)
    gate_post_t, up_post_t, down_post_all = (
        second[:, k * unit : (k + 1) * unit].reshape(ny * unit, width) for k in range(3)
    )
    mixers = jnp.concatenate(
        [
            second[:, 3 * unit + k * kept : 3 * unit + (k + 1) * kept].reshape(ny * kept, width)
            for k in range(4)
        ],
        axis=1,
    )
    part, residual, gate_post_t, up_post_t, down_post_all, mixers, gain_block = (
        lax.optimization_barrier(
            (part, residual, gate_post_t, up_post_t, down_post_all, mixers, gain_block)
        )
    )
    branch = exchanged(part.reshape(nz, piece, rows), "z")
    branch = branch.astype(f32).sum(axis=0)
    stream_piece = (residual.astype(f32) + 0.5 * branch).astype(bf16)

    stream_t = gathered(stream_piece, TP).reshape(block, rows)
    widened = stream_t.astype(f32)
    squares = jnp.sum(widened * widened, axis=0)
    scaled = reordered(widened.reshape(ny, kept, rows), odd, upper).reshape(block, rows)
    scaled = (scaled * gain_block[:, None]).astype(bf16)
    heads = width // HEAD_DIM
    parts = dot(scaled, mixers, 0, 0).astype(bf16)
    parts = parts.reshape(nz, own, 4 * heads, HEAD_DIM).swapaxes(1, 2)
    note = jnp.where(
        mine,
        stream_t.T.reshape(nz, own, block),
        jnp.broadcast_to(squares.astype(bf16).reshape(nz, own, 1), (nz, own, block)),
    )
    message = jnp.concatenate([parts.reshape(nz, 4 * heads * own, HEAD_DIM), note], axis=1)
    arrived = exchanged(message, "z")
    projected = arrived[:, : 4 * heads * own].astype(f32).sum(axis=0)
    notes = arrived[:, 4 * heads * own :]
    stream_a = lax.dynamic_slice_in_dim(notes, note_at, halves, axis=0)
    stream_a = stream_a.swapaxes(0, 1).reshape(own, width).astype(f32)
    total = jnp.sum(jnp.where(elsewhere, notes[:, :, 0].astype(f32), 0.0), axis=0)
    total = total + jnp.sum(stream_a * stream_a, axis=1)
    projected = projected.reshape(4, heads, own, HEAD_DIM)
    projected = projected * lax.rsqrt(total / D + EPSILON)[:, None]

    query_pre, forget_pre, value_pre, outgate_pre = (
        projected[k].swapaxes(0, 1) for k in range(4)
    )
    log_keep = jnp.logaddexp(log_floor, log_rest + jax.nn.log_sigmoid(forget_pre))
    inject = rest_rate * jax.nn.sigmoid(-forget_pre)
    next_state = (
        jnp.exp(log_keep)[..., None] * memory_state + inject[..., None] * value_pre[:, :, None, :]
    )
    readout = jnp.einsum(
        "bhk,bhkv->bhv", jax.nn.silu(query_pre), next_state, precision=lax.Precision.HIGHEST
    )
    normed = (
        readout
        * lax.rsqrt(jnp.mean(readout * readout, axis=2, keepdims=True) + EPSILON)
        * head_gain.reshape(heads, HEAD_DIM)
    )
    mixed_heads = (normed * jax.nn.silu(outgate_pre)).reshape(own, width).astype(bf16)
    partial_out = dot(mixed_heads, out_weight, 1, 0).astype(bf16)
    mixed = exchanged(partial_out.reshape(own, tp, width).swapaxes(0, 1), TP)
    stream_b = (stream_a + mixed.astype(f32).sum(axis=0)).astype(bf16)

    all_rows = gathered(stream_b, "z").reshape(rows, width)
    hidden, _ = hidden_units(all_rows, gain_post, gate_post_t, up_post_t, (), lambda _: (), ())
    part = dot(hidden, down_post_all, 0, 0).astype(bf16)
    branch = exchanged(part.reshape(nz, own, width), "z").astype(f32).sum(axis=0)
    layer_out = (stream_b.astype(f32) + 0.5 * branch).astype(bf16)
    return (layer_out, next_state)


def solution(mesh):
    grid = Mesh(mesh.devices.reshape(16, 4, 4, 2), ("z", "y", "x", "c"))
    kv = ("z", "y")
    in_specs = (
        P(kv, TP),
        P(TP),
        P(TP, kv),
        P(TP, kv),
        P(kv, TP),
        P(),
        P(kv, TP),
        P(kv, TP),
        P(kv, TP),
        P(kv, TP),
        P(TP),
        P(TP),
        P(TP, None),
        P(TP),
        P(TP, kv),
        P(TP, kv),
        P(kv, TP),
        P(kv, TP, None, None),
    )
    out_specs = (P(kv, TP), P(kv, TP, None, None))

    return jax.shard_map(shards, mesh=grid, in_specs=in_specs, out_specs=out_specs, check_vma=False)
```

```python
import jax
import jax.numpy as jnp
from jax import lax
from jax.experimental import pallas as pl
from jax.experimental.pallas import tpu as pltpu
from jax.sharding import Mesh, PartitionSpec as P

D = 2048
HEAD_DIM = 128
EPSILON = 1e-06
TP = ("x", "c")

f32 = jnp.float32
bf16 = jnp.bfloat16


def exchanged(tiles, axis, groups=None):
    return lax.all_to_all(
        tiles, axis, split_axis=0, concat_axis=0, axis_index_groups=groups, tiled=True
    )


def gathered(array, axis):
    return exchanged(jnp.broadcast_to(array, (lax.axis_size(axis), *array.shape)), axis)


def dot(a, b, da, db):
    return lax.dot_general(a, b, (((da,), (db,)), ((), ())), preferred_element_type=f32)


def from_others(array, axis):
    n = lax.axis_size(axis)
    later = [
        lax.ppermute(array, axis, [(i, (i - k) % n) for i in range(n)]) for k in range(1, n)
    ]
    return [array, *later]


def staged(unit, copies, ups, downs, kept, small):
    rows, gate_a, up_a, down_a, gate_b, up_b, down_b, *projections = ups + downs + kept
    units, width = gate_a.shape
    height = projections[0].shape[0]
    n_in = 7 + len(projections) + len(small)

    def kernel(*refs):
        ins, outs = refs[:n_in], refs[n_in : n_in + 3 + len(small)]
        held, sems = refs[-2], refs[-1]
        spread, first, second = outs[:3]
        moves = [(ins[0], held)]
        moves += [(ins[1 + k], first.at[pl.ds(k * unit, units)]) for k in range(3)]
        moves += [(ins[4 + k], second.at[pl.ds(k * unit, units)]) for k in range(3)]
        for k in range(len(projections)):
            moves.append((ins[7 + k], second.at[pl.ds(3 * unit + k * height, height)]))
        for k in range(len(small)):
            moves.append((ins[7 + len(projections) + k], outs[3 + k]))
        started = [pltpu.make_async_copy(a, b, sems.at[k]) for k, (a, b) in enumerate(moves)]
        for move in started:
            move.start()
        if unit > units:
            blank = jnp.zeros((unit - units, width), first.dtype)
            for k in range(3):
                first[pl.ds(k * unit + units, unit - units), :] = blank
                second[pl.ds(k * unit + units, unit - units), :] = blank
        started[0].wait()
        for k in range(copies):
            spread[k] = held[...]
        for move in started[1:]:
            move.wait()

    arrays = [rows, gate_a, up_a, down_a, gate_b, up_b, down_b, *projections, *small]
    vmem = pl.BlockSpec(memory_space=pltpu.VMEM)
    shapes = [
        jax.ShapeDtypeStruct((copies, *rows.shape), bf16),
        jax.ShapeDtypeStruct((3 * unit, width), bf16),
        jax.ShapeDtypeStruct((3 * unit + len(projections) * height, width), bf16),
        *[jax.ShapeDtypeStruct(v.shape, v.dtype) for v in small],
    ]
    return pl.pallas_call(
        kernel,
        out_shape=shapes,
        in_specs=[pl.BlockSpec(memory_space=pl.ANY)] * n_in,
        out_specs=[vmem] * len(shapes),
        scratch_shapes=[pltpu.VMEM(rows.shape, bf16), pltpu.SemaphoreType.DMA((n_in,))],
    )(*arrays)


def doubled(array, axis, apart):
    n = lax.axis_size(axis)
    return jnp.concatenate([array, lax.ppermute(array, axis, [(i, i ^ apart) for i in range(n)])])


def reordered(blocks, odd, upper):
    blocks = jnp.stack([blocks[0], blocks[2], blocks[1], blocks[3]])
    halves = jnp.concatenate([blocks[2:], blocks[:2]])
    blocks = jnp.where(odd, halves, blocks)
    pairs = jnp.concatenate([blocks[1:2], blocks[0:1], blocks[3:4], blocks[2:3]])
    return jnp.where(upper, pairs, blocks)


def hidden_units(rows, gain_vec, gate_t, up_t, extra, finish, later):
    tp = lax.axis_size(TP)
    n = rows.shape[0]
    widened = rows.astype(f32)
    squares = jnp.sum(widened * widened, axis=1)
    scaled = (widened * gain_vec).astype(bf16)
    gate_part = dot(gate_t, scaled, 1, 1).astype(bf16)
    up_part = dot(up_t, scaled, 1, 1).astype(bf16)
    unit = gate_part.shape[0] // tp
    tiles = [
        gate_part.reshape(tp, unit, n),
        up_part.reshape(tp, unit, n),
        jnp.broadcast_to(squares.astype(bf16), (tp, 8, n)),
        *extra,
    ]
    message, *later = lax.optimization_barrier((jnp.concatenate(tiles, axis=1), *later))
    arrived = exchanged(message, TP)
    summed = arrived[:, : 2 * unit + 8].astype(f32).sum(axis=0)
    inverse = lax.rsqrt(summed[2 * unit] / D + EPSILON)[None, :]
    hidden = (jax.nn.silu(summed[:unit] * inverse) * (summed[unit : 2 * unit] * inverse)).astype(bf16)
    hidden, *rest = lax.optimization_barrier((hidden, *finish(arrived[:, 2 * unit + 8 :]), *later))
    every = gathered(hidden, TP).reshape(tp * unit, n)
    return every, rest


def shards(
    residual_in,
    gain_pre,
    gate_pre,
    up_pre,
    down_pre,
    gain_mix,
    query_weight,
    forget_weight,
    value_weight,
    outgate_weight,
    lower_bound,
    head_gain,
    out_weight,
    gain_post,
    gate_post,
    up_post,
    down_post,
    memory_state,
):
    nz, ny, tp = lax.axis_size("z"), lax.axis_size("y"), lax.axis_size(TP)
    z_at, t_at, y_at = (lax.axis_index(k).astype(jnp.uint32) for k in ("z", TP, "y"))
    own, width = residual_in.shape
    rows = nz * own
    units = gate_pre.shape[1]
    unit = -(-units * ny // (8 * tp)) * 8 * tp // ny
    block = width * tp // nz
    piece = block // tp
    halves = width // block
    kept = query_weight.shape[0]

    spread, first, second, gain_pre, gain_post, head_gain, lower_bound, gain_mix = staged(
        unit,
        nz,
        [residual_in, gate_pre.T, up_pre.T],
        [down_pre, gate_post.T, up_post.T, down_post],
        [query_weight, forget_weight, value_weight, outgate_weight],
        [v.reshape(-1, HEAD_DIM) for v in (gain_pre, gain_post, head_gain, lower_bound, gain_mix)],
    )
    gain_pre, gain_post = gain_pre.reshape(width), gain_post.reshape(width)
    gain_block = lax.dynamic_slice_in_dim(gain_mix, z_at * block // HEAD_DIM, block // HEAD_DIM)
    gain_block = reordered(gain_block.reshape(ny, kept), y_at % 2 == 1, y_at // 2 == 1).reshape(block)
    first = from_others(first, "y")
    second = doubled(second, "y", 2)
    middle = [*range(nz // 2, nz), *range(nz // 2)]
    all_rows = exchanged(spread, "z", [middle])
    all_rows = jnp.concatenate([all_rows[nz // 2 :], all_rows[: nz // 2]])
    first = jnp.stack(first)
    down_tiles = first[:, 2 * unit :].swapaxes(1, 2).reshape(ny, halves, tp, piece, unit)
    down_tiles = down_tiles.transpose(2, 0, 1, 3, 4).reshape(tp, ny * halves * piece, unit)
    mine = z_at // halves == t_at
    elsewhere = (jnp.arange(nz, dtype=jnp.uint32) // halves != t_at)[:, None]
    note_at = t_at * halves
    odd, upper = y_at % 2 == 1, y_at // 2 == 1
    floor_rate = lower_bound.reshape(-1, HEAD_DIM)
    floors = (jnp.log(floor_rate), jnp.log1p(-floor_rate), 1.0 - floor_rate)
    all_rows, second, first, down_tiles, *known = lax.optimization_barrier(
        (all_rows, second, first, down_tiles, gain_block, gain_pre, gain_post, head_gain)
        + (*floors, mine, elsewhere, note_at, odd, upper, z_at)
    )
    gain_block, gain_pre, gain_post, head_gain, log_floor, log_rest, rest_rate = known[:7]
    mine, elsewhere, note_at, odd, upper, z_at = known[7:]
    others = lax.ppermute(second, "y", [(i, i ^ 1) for i in range(ny)])
    gate_pre_t = first[:, :unit].reshape(ny * unit, width)
    up_pre_t = first[:, unit : 2 * unit].reshape(ny * unit, width)

    all_rows = all_rows.reshape(rows, width)
    turned = all_rows.T.reshape(halves, tp, piece, rows).swapaxes(0, 1)
    own_rows = (tp, halves * piece, rows)

    def finish(extra):
        pieces = extra[:, : halves * piece].reshape(nz, piece, rows)
        return (
            lax.dynamic_index_in_dim(pieces, z_at, axis=0, keepdims=False),
            *[extra[:, k * halves * piece :][:, : halves * piece].reshape(width, unit) for k in range(1, ny + 1)],
        )

    hidden, (residual, *down_pre_t, second, gain_block) = hidden_units(
        all_rows,
        gain_pre,
        gate_pre_t,
        up_pre_t,
        (turned.reshape(own_rows), down_tiles),
        finish,
        (second, gain_block),
    )
    part = sum(
        dot(down_pre_t[k], hidden[k * unit : (k + 1) * unit], 1, 0) for k in range(ny)
    ).astype(bf16)
    second = jnp.concatenate([second, others]).reshape(ny, -1, width)
    gate_post_t, up_post_t, down_post_all = (
        second[:, k * unit : (k + 1) * unit].reshape(ny * unit, width) for k in range(3)
    )
    mixers = jnp.concatenate(
        [
            second[:, 3 * unit + k * kept : 3 * unit + (k + 1) * kept].reshape(ny * kept, width)
            for k in range(4)
        ],
        axis=1,
    )
    part, residual, gate_post_t, up_post_t, down_post_all, mixers, gain_block = (
        lax.optimization_barrier(
            (part, residual, gate_post_t, up_post_t, down_post_all, mixers, gain_block)
        )
    )
    branch = exchanged(part.reshape(nz, piece, rows), "z")
    branch = branch.astype(f32).sum(axis=0)
    stream_piece = (residual.astype(f32) + 0.5 * branch).astype(bf16)

    stream_t = gathered(stream_piece, TP).reshape(block, rows)
    widened = stream_t.astype(f32)
    squares = jnp.sum(widened * widened, axis=0)
    scaled = reordered(widened.reshape(ny, kept, rows), odd, upper).reshape(block, rows)
    scaled = (scaled * gain_block[:, None]).astype(bf16)
    heads = width // HEAD_DIM
    parts = dot(scaled, mixers, 0, 0).astype(bf16)
    parts = parts.reshape(nz, own, 4 * heads, HEAD_DIM).swapaxes(1, 2)
    note = jnp.where(
        mine,
        stream_t.T.reshape(nz, own, block),
        jnp.broadcast_to(squares.astype(bf16).reshape(nz, own, 1), (nz, own, block)),
    )
    message = jnp.concatenate([parts.reshape(nz, 4 * heads * own, HEAD_DIM), note], axis=1)
    arrived = exchanged(message, "z")
    projected = arrived[:, : 4 * heads * own].astype(f32).sum(axis=0)
    notes = arrived[:, 4 * heads * own :]
    stream_a = lax.dynamic_slice_in_dim(notes, note_at, halves, axis=0)
    stream_a = stream_a.swapaxes(0, 1).reshape(own, width).astype(f32)
    total = jnp.sum(jnp.where(elsewhere, notes[:, :, 0].astype(f32), 0.0), axis=0)
    total = total + jnp.sum(stream_a * stream_a, axis=1)
    projected = projected.reshape(4, heads, own, HEAD_DIM)
    projected = projected * lax.rsqrt(total / D + EPSILON)[:, None]

    query_pre, forget_pre, value_pre, outgate_pre = (
        projected[k].swapaxes(0, 1) for k in range(4)
    )
    log_keep = jnp.logaddexp(log_floor, log_rest + jax.nn.log_sigmoid(forget_pre))
    inject = rest_rate * jax.nn.sigmoid(-forget_pre)
    next_state = (
        jnp.exp(log_keep)[..., None] * memory_state + inject[..., None] * value_pre[:, :, None, :]
    )
    readout = jnp.einsum(
        "bhk,bhkv->bhv", jax.nn.silu(query_pre), next_state, precision=lax.Precision.HIGHEST
    )
    normed = (
        readout
        * lax.rsqrt(jnp.mean(readout * readout, axis=2, keepdims=True) + EPSILON)
        * head_gain.reshape(heads, HEAD_DIM)
    )
    mixed_heads = (normed * jax.nn.silu(outgate_pre)).reshape(own, width).astype(bf16)
    partial_out = dot(mixed_heads, out_weight, 1, 0).astype(bf16)
    mixed = exchanged(partial_out.reshape(own, tp, width).swapaxes(0, 1), TP)
    stream_b = (stream_a + mixed.astype(f32).sum(axis=0)).astype(bf16)

    all_rows = gathered(stream_b, "z").reshape(rows, width)
    hidden, _ = hidden_units(all_rows, gain_post, gate_post_t, up_post_t, (), lambda _: (), ())
    part = dot(hidden, down_post_all, 0, 0).astype(bf16)
    branch = exchanged(part.reshape(nz, own, width), "z").astype(f32).sum(axis=0)
    layer_out = (stream_b.astype(f32) + 0.5 * branch).astype(bf16)
    return (layer_out, next_state)


def solution(mesh):
    grid = Mesh(mesh.devices.reshape(16, 4, 4, 2), ("z", "y", "x", "c"))
    kv = ("z", "y")
    in_specs = (
        P(kv, TP),
        P(TP),
        P(TP, kv),
        P(TP, kv),
        P(kv, TP),
        P(),
        P(kv, TP),
        P(kv, TP),
        P(kv, TP),
        P(kv, TP),
        P(TP),
        P(TP),
        P(TP, None),
        P(TP),
        P(TP, kv),
        P(TP, kv),
        P(kv, TP),
        P(kv, TP, None, None),
    )
    out_specs = (P(kv, TP), P(kv, TP, None, None))

    return jax.shard_map(shards, mesh=grid, in_specs=in_specs, out_specs=out_specs, check_vma=False)
```

```python
import jax
import jax.numpy as jnp
from jax import lax
from jax.experimental import pallas as pl
from jax.experimental.pallas import tpu as pltpu
from jax.sharding import Mesh, PartitionSpec as P

D = 2048
HEAD_DIM = 128
EPSILON = 1e-06
TP = ("x", "c")

f32 = jnp.float32
bf16 = jnp.bfloat16


def exchanged(tiles, axis, groups=None):
    return lax.all_to_all(
        tiles, axis, split_axis=0, concat_axis=0, axis_index_groups=groups, tiled=True
    )


def gathered(array, axis):
    return exchanged(jnp.broadcast_to(array, (lax.axis_size(axis), *array.shape)), axis)


def dot(a, b, da, db):
    return lax.dot_general(a, b, (((da,), (db,)), ((), ())), preferred_element_type=f32)


def from_others(array, axis):
    n = lax.axis_size(axis)
    later = [
        lax.ppermute(array, axis, [(i, (i - k) % n) for i in range(n)]) for k in range(1, n)
    ]
    return [array, *later]


def staged(unit, copies, at, ups, downs, kept, small, floor_rate, gains):
    rows, gate_a, up_a, down_a, gate_b, up_b, down_b, *projections = ups + downs + kept
    units, width = gate_a.shape
    height = projections[0].shape[0]
    n_in = 9 + len(projections) + len(small)

    def kernel(at_ref, *refs):
        ins, outs = refs[:n_in], refs[n_in:-4]
        held, held_floor, held_gains, sems = refs[-4:]
        spread, first, second = outs[:3]
        gain_block, log_floor, log_rest, rest = outs[3 + len(small) :]
        moves = [(ins[0], held)]
        moves += [(ins[1 + k], first.at[pl.ds(k * unit, units)]) for k in range(3)]
        moves += [(ins[4 + k], second.at[pl.ds(k * unit, units)]) for k in range(3)]
        for k in range(len(projections)):
            moves.append((ins[7 + k], second.at[pl.ds(3 * unit + k * height, height)]))
        for k in range(len(small)):
            moves.append((ins[7 + len(projections) + k], outs[3 + k]))
        moves += [(ins[-2], held_floor), (ins[-1], held_gains)]
        started = [pltpu.make_async_copy(a, b, sems.at[k]) for k, (a, b) in enumerate(moves)]
        for move in started:
            move.start()
        if unit > units:
            blank = jnp.zeros((unit - units, width), first.dtype)
            for k in range(3):
                first[pl.ds(k * unit + units, unit - units), :] = blank
                second[pl.ds(k * unit + units, unit - units), :] = blank
        started[0].wait()
        for k in range(copies):
            spread[k] = held[...]
        for move in started[1:]:
            move.wait()
        gain_block[...] = held_gains[pl.ds(at_ref[0], 1), :]
        floor = held_floor[...]
        log_floor[...] = jnp.log(floor)
        log_rest[...] = jnp.log1p(-floor)
        rest[...] = 1.0 - floor

    arrays = [rows, gate_a, up_a, down_a, gate_b, up_b, down_b, *projections, *small]
    arrays += [floor_rate, gains]
    vmem = pl.BlockSpec(memory_space=pltpu.VMEM)
    shapes = [
        jax.ShapeDtypeStruct((copies, *rows.shape), bf16),
        jax.ShapeDtypeStruct((3 * unit, width), bf16),
        jax.ShapeDtypeStruct((3 * unit + len(projections) * height, width), bf16),
        *[jax.ShapeDtypeStruct(v.shape, v.dtype) for v in small],
        jax.ShapeDtypeStruct((1, gains.shape[1]), f32),
        *[jax.ShapeDtypeStruct(floor_rate.shape, f32)] * 3,
    ]
    return pl.pallas_call(
        kernel,
        out_shape=shapes,
        in_specs=[pl.BlockSpec(memory_space=pltpu.SMEM)]
        + [pl.BlockSpec(memory_space=pl.ANY)] * n_in,
        out_specs=[vmem] * len(shapes),
        scratch_shapes=[
            pltpu.VMEM(rows.shape, bf16),
            pltpu.VMEM(floor_rate.shape, f32),
            pltpu.VMEM(gains.shape, f32),
            pltpu.SemaphoreType.DMA((n_in,)),
        ],
    )(at, *arrays)


def reordered(blocks, odd, upper):
    blocks = jnp.stack([blocks[0], blocks[2], blocks[1], blocks[3]])
    halves = jnp.concatenate([blocks[2:], blocks[:2]])
    blocks = jnp.where(odd, halves, blocks)
    pairs = jnp.concatenate([blocks[1:2], blocks[0:1], blocks[3:4], blocks[2:3]])
    return jnp.where(upper, pairs, blocks)


def hidden_units(rows, gain_vec, gate_t, up_t, extra, finish, later):
    tp = lax.axis_size(TP)
    n = rows.shape[0]
    widened = rows.astype(f32)
    squares = jnp.sum(widened * widened, axis=1)
    scaled = (widened * gain_vec).astype(bf16)
    gate_part = dot(gate_t, scaled, 1, 1).astype(bf16)
    up_part = dot(up_t, scaled, 1, 1).astype(bf16)
    unit = gate_part.shape[0] // tp
    tiles = [
        gate_part.reshape(tp, unit, n),
        up_part.reshape(tp, unit, n),
        jnp.broadcast_to(squares.astype(bf16), (tp, 8, n)),
        *extra,
    ]
    message, *later = lax.optimization_barrier((jnp.concatenate(tiles, axis=1), *later))
    arrived = exchanged(message, TP)
    summed = arrived[:, : 2 * unit + 8].astype(f32).sum(axis=0)
    inverse = lax.rsqrt(summed[2 * unit] / D + EPSILON)[None, :]
    hidden = (jax.nn.silu(summed[:unit] * inverse) * (summed[unit : 2 * unit] * inverse)).astype(bf16)
    hidden, *rest = lax.optimization_barrier((hidden, *finish(arrived[:, 2 * unit + 8 :]), *later))
    every = gathered(hidden, TP).reshape(tp * unit, n)
    return every, rest


def shards(
    residual_in,
    gain_pre,
    gate_pre,
    up_pre,
    down_pre,
    gain_mix,
    query_weight,
    forget_weight,
    value_weight,
    outgate_weight,
    lower_bound,
    head_gain,
    out_weight,
    gain_post,
    gate_post,
    up_post,
    down_post,
    memory_state,
):
    nz, ny, tp = lax.axis_size("z"), lax.axis_size("y"), lax.axis_size(TP)
    z_at, t_at, y_at = (lax.axis_index(k).astype(jnp.uint32) for k in ("z", TP, "y"))
    own, width = residual_in.shape
    rows = nz * own
    units = gate_pre.shape[1]
    unit = -(-units * ny // (8 * tp)) * 8 * tp // ny
    block = width * tp // nz
    piece = block // tp
    halves = width // block
    kept = query_weight.shape[0]

    spread, first, second, gain_pre, gain_post, head_gain, gain_block, *floors = staged(
        unit,
        nz,
        z_at.astype(jnp.int32)[None],
        [residual_in, gate_pre.T, up_pre.T],
        [down_pre, gate_post.T, up_post.T, down_post],
        [query_weight, forget_weight, value_weight, outgate_weight],
        [v.reshape(-1, HEAD_DIM) for v in (gain_pre, gain_post, head_gain)],
        lower_bound.reshape(-1, HEAD_DIM),
        gain_mix.reshape(-1, block),
    )
    gain_pre, gain_post = gain_pre.reshape(width), gain_post.reshape(width)
    gain_block = reordered(gain_block.reshape(ny, kept), y_at % 2 == 1, y_at // 2 == 1).reshape(block)
    first = from_others(first, "y")
    middle = [*range(nz // 2, nz), *range(nz // 2)]
    all_rows = exchanged(spread, "z", [middle])
    all_rows = jnp.concatenate([all_rows[nz // 2 :], all_rows[: nz // 2]])
    first = jnp.stack(first)
    down_tiles = first[:, 2 * unit :].swapaxes(1, 2).reshape(ny, halves, tp, piece, unit)
    down_tiles = down_tiles.transpose(2, 0, 1, 3, 4).reshape(tp, ny * halves * piece, unit)
    mine = z_at // halves == t_at
    elsewhere = (jnp.arange(nz, dtype=jnp.uint32) // halves != t_at)[:, None]
    note_at = t_at * halves
    odd, upper = y_at % 2 == 1, y_at // 2 == 1
    all_rows, second, first, down_tiles, *known = lax.optimization_barrier(
        (all_rows, second, first, down_tiles, gain_block, gain_pre, gain_post, head_gain)
        + (*floors, mine, elsewhere, note_at, odd, upper, z_at)
    )
    gain_block, gain_pre, gain_post, head_gain, log_floor, log_rest, rest_rate = known[:7]
    mine, elsewhere, note_at, odd, upper, z_at = known[7:]
    others = lax.ppermute(second, "y", [(i, i ^ 2) for i in range(ny)])
    gate_pre_t = first[:, :unit].reshape(ny * unit, width)
    up_pre_t = first[:, unit : 2 * unit].reshape(ny * unit, width)

    all_rows = all_rows.reshape(rows, width)
    turned = all_rows.T.reshape(halves, tp, piece, rows).swapaxes(0, 1)
    own_rows = (tp, halves * piece, rows)

    def finish(extra):
        pieces = extra[:, : halves * piece].reshape(nz, piece, rows)
        return (
            lax.dynamic_index_in_dim(pieces, z_at, axis=0, keepdims=False),
            jnp.concatenate([second, others]),
            *[extra[:, k * halves * piece :][:, : halves * piece].reshape(width, unit) for k in range(1, ny + 1)],
        )

    hidden, (residual, second, *down_pre_t, gain_block) = hidden_units(
        all_rows,
        gain_pre,
        gate_pre_t,
        up_pre_t,
        (turned.reshape(own_rows), down_tiles),
        finish,
        (gain_block,),
    )
    part = sum(
        dot(down_pre_t[k], hidden[k * unit : (k + 1) * unit], 1, 0) for k in range(ny)
    ).astype(bf16)
    part, residual, second, gain_block = lax.optimization_barrier(
        (part, residual, second, gain_block)
    )
    others = lax.ppermute(second, "y", [(i, i ^ 1) for i in range(ny)])
    branch = exchanged(part.reshape(nz, piece, rows), "z")
    branch = branch.astype(f32).sum(axis=0)
    stream_piece = (residual.astype(f32) + 0.5 * branch).astype(bf16)

    second = jnp.concatenate([second, others]).reshape(ny, -1, width)
    gate_post_t, up_post_t, down_post_all = (
        second[:, k * unit : (k + 1) * unit].reshape(ny * unit, width) for k in range(3)
    )
    mixers = jnp.concatenate(
        [
            second[:, 3 * unit + k * kept : 3 * unit + (k + 1) * kept].reshape(ny * kept, width)
            for k in range(4)
        ],
        axis=1,
    )
    stream_piece, gate_post_t, up_post_t, down_post_all, mixers = lax.optimization_barrier(
        (stream_piece, gate_post_t, up_post_t, down_post_all, mixers)
    )
    stream_t = gathered(stream_piece, TP).reshape(block, rows)
    widened = stream_t.astype(f32)
    squares = jnp.sum(widened * widened, axis=0)
    scaled = reordered(widened.reshape(ny, kept, rows), odd, upper).reshape(block, rows)
    scaled = (scaled * gain_block[:, None]).astype(bf16)
    heads = width // HEAD_DIM
    parts = dot(scaled, mixers, 0, 0).astype(bf16)
    parts = parts.reshape(nz, own, 4 * heads, HEAD_DIM).swapaxes(1, 2)
    note = jnp.where(
        mine,
        stream_t.T.reshape(nz, own, block),
        jnp.broadcast_to(squares.astype(bf16).reshape(nz, own, 1), (nz, own, block)),
    )
    message = jnp.concatenate([parts.reshape(nz, 4 * heads * own, HEAD_DIM), note], axis=1)
    arrived = exchanged(message, "z")
    projected = arrived[:, : 4 * heads * own].astype(f32).sum(axis=0)
    notes = arrived[:, 4 * heads * own :]
    stream_a = lax.dynamic_slice_in_dim(notes, note_at, halves, axis=0)
    stream_a = stream_a.swapaxes(0, 1).reshape(own, width).astype(f32)
    total = jnp.sum(jnp.where(elsewhere, notes[:, :, 0].astype(f32), 0.0), axis=0)
    total = total + jnp.sum(stream_a * stream_a, axis=1)
    projected = projected.reshape(4, heads, own, HEAD_DIM)
    projected = projected * lax.rsqrt(total / D + EPSILON)[:, None]

    query_pre, forget_pre, value_pre, outgate_pre = (
        projected[k].swapaxes(0, 1) for k in range(4)
    )
    log_keep = jnp.logaddexp(log_floor, log_rest + jax.nn.log_sigmoid(forget_pre))
    inject = rest_rate * jax.nn.sigmoid(-forget_pre)
    next_state = (
        jnp.exp(log_keep)[..., None] * memory_state + inject[..., None] * value_pre[:, :, None, :]
    )
    readout = jnp.einsum(
        "bhk,bhkv->bhv", jax.nn.silu(query_pre), next_state, precision=lax.Precision.HIGHEST
    )
    normed = (
        readout
        * lax.rsqrt(jnp.mean(readout * readout, axis=2, keepdims=True) + EPSILON)
        * head_gain.reshape(heads, HEAD_DIM)
    )
    mixed_heads = (normed * jax.nn.silu(outgate_pre)).reshape(own, width).astype(bf16)
    partial_out = dot(mixed_heads, out_weight, 1, 0).astype(bf16)
    mixed = exchanged(partial_out.reshape(own, tp, width).swapaxes(0, 1), TP)
    stream_b = (stream_a + mixed.astype(f32).sum(axis=0)).astype(bf16)

    all_rows = gathered(stream_b, "z").reshape(rows, width)
    hidden, _ = hidden_units(all_rows, gain_post, gate_post_t, up_post_t, (), lambda _: (), ())
    part = dot(hidden, down_post_all, 0, 0).astype(bf16)
    branch = exchanged(part.reshape(nz, own, width), "z").astype(f32).sum(axis=0)
    layer_out = (stream_b.astype(f32) + 0.5 * branch).astype(bf16)
    return (layer_out, next_state)


def solution(mesh):
    grid = Mesh(mesh.devices.reshape(16, 4, 4, 2), ("z", "y", "x", "c"))
    kv = ("z", "y")
    in_specs = (
        P(kv, TP),
        P(TP),
        P(TP, kv),
        P(TP, kv),
        P(kv, TP),
        P(),
        P(kv, TP),
        P(kv, TP),
        P(kv, TP),
        P(kv, TP),
        P(TP),
        P(TP),
        P(TP, None),
        P(TP),
        P(TP, kv),
        P(TP, kv),
        P(kv, TP),
        P(kv, TP, None, None),
    )
    out_specs = (P(kv, TP), P(kv, TP, None, None))

    return jax.shard_map(shards, mesh=grid, in_specs=in_specs, out_specs=out_specs, check_vma=False)
```

```python
import jax
import jax.numpy as jnp
from jax import lax
from jax.experimental import pallas as pl
from jax.experimental.pallas import tpu as pltpu
from jax.sharding import Mesh, PartitionSpec as P

D = 2048
HEAD_DIM = 128
EPSILON = 1e-06
TP = ("x", "c")

f32 = jnp.float32
bf16 = jnp.bfloat16


def exchanged(tiles, axis, groups=None):
    return lax.all_to_all(
        tiles, axis, split_axis=0, concat_axis=0, axis_index_groups=groups, tiled=True
    )


def gathered(array, axis):
    return exchanged(jnp.broadcast_to(array, (lax.axis_size(axis), *array.shape)), axis)


def dot(a, b, da, db):
    return lax.dot_general(a, b, (((da,), (db,)), ((), ())), preferred_element_type=f32)


def from_later(array, axis, k):
    n = lax.axis_size(axis)
    return lax.ppermute(array, axis, [(i, (i - k) % n) for i in range(n)])


def staged(unit, copies, at, ups, downs, kept, vectors, floor_rate, gains):
    rows, gate_a, up_a, down_a, gate_b, up_b, down_b, *projections = ups + downs + kept
    units, width = gate_a.shape
    height = projections[0].shape[0]
    wide, lanes = floor_rate.shape
    arrays = [rows, gate_a, up_a, down_a, gate_b, up_b, down_b, *projections, *vectors]
    arrays += [floor_rate, gains]
    n_in, n_held = len(arrays), len(vectors) + 2

    def kernel(at_ref, *refs):
        ins, (spread, stack, small) = refs[:n_in], refs[n_in : n_in + 3]
        held, kept_small, sems = refs[n_in + 3], refs[n_in + 4 : -1], refs[-1]
        moves = [(ins[0], held)]
        moves += [(ins[1 + k], stack.at[pl.ds(k * unit, units)]) for k in range(6)]
        for k in range(len(projections)):
            moves.append((ins[7 + k], stack.at[pl.ds(6 * unit + k * height, height)]))
        moves += list(zip(ins[n_in - n_held :], kept_small))
        started = [pltpu.make_async_copy(a, b, sems.at[k]) for k, (a, b) in enumerate(moves)]
        for move in started:
            move.start()
        if unit > units:
            blank = jnp.zeros((unit - units, width), stack.dtype)
            for k in range(6):
                stack[pl.ds(k * unit + units, unit - units), :] = blank
        started[0].wait()
        for k in range(copies):
            spread[k] = held[...]
        for move in started[1:]:
            move.wait()
        floor = kept_small[-2][...]
        lines = [ref[...] for ref in kept_small[:-2]]
        lines += [jnp.log(floor), jnp.log1p(-floor), 1.0 - floor]
        small[...] = jnp.zeros(small.shape, f32)
        for k, line in enumerate(lines):
            small[pl.ds(k * wide, wide), :] = line
        small[pl.ds(len(lines) * wide, 1), :] = kept_small[-1][pl.ds(at_ref[0], 1), :]

    n_small = -(-((len(vectors) + 3) * wide + 1) // 8) * 8
    shapes = [
        jax.ShapeDtypeStruct((copies, *rows.shape), bf16),
        pltpu.VMEM((6 * unit + len(projections) * height, width), bf16),
        pltpu.VMEM((n_small, lanes), f32),
    ]
    return pl.pallas_call(
        kernel,
        out_shape=shapes,
        in_specs=[pl.BlockSpec(memory_space=pltpu.SMEM)]
        + [pl.BlockSpec(memory_space=pl.ANY)] * n_in,
        out_specs=[pl.BlockSpec(memory_space=pltpu.VMEM)] * len(shapes),
        scratch_shapes=[pltpu.VMEM(rows.shape, bf16)]
        + [pltpu.VMEM(v.shape, f32) for v in (*vectors, floor_rate, gains)]
        + [pltpu.SemaphoreType.DMA((n_in,))],
    )(at, *arrays)


def reordered(array, odd, upper):
    parts = jnp.split(array, 4)
    parts = [jnp.where(odd, parts[(k + 1) % 4], parts[k]) for k in range(4)]
    return jnp.concatenate([jnp.where(upper, parts[(k + 2) % 4], parts[k]) for k in range(4)])


def hidden_units(rows, gain_vec, gate_t, up_t, extra, finish, later):
    tp = lax.axis_size(TP)
    n = rows.shape[0]
    widened = rows.astype(f32)
    squares = jnp.sum(widened * widened, axis=1)
    scaled = (widened * gain_vec).astype(bf16)
    gate_part = dot(gate_t, scaled, 1, 1).astype(bf16)
    up_part = dot(up_t, scaled, 1, 1).astype(bf16)
    unit = gate_part.shape[0] // tp
    tiles = [
        gate_part.reshape(tp, unit, n),
        up_part.reshape(tp, unit, n),
        jnp.broadcast_to(squares.astype(bf16), (tp, 8, n)),
        *extra,
    ]
    message, *later = lax.optimization_barrier((jnp.concatenate(tiles, axis=1), *later))
    arrived = exchanged(message, TP)
    summed = arrived[:, : 2 * unit + 8].astype(f32).sum(axis=0)
    inverse = lax.rsqrt(summed[2 * unit] / D + EPSILON)[None, :]
    hidden = (jax.nn.silu(summed[:unit] * inverse) * (summed[unit : 2 * unit] * inverse)).astype(bf16)
    hidden, *rest = lax.optimization_barrier((hidden, *finish(arrived[:, 2 * unit + 8 :]), *later))
    every = gathered(hidden, TP).reshape(tp * unit, n)
    return every, rest


def shards(
    residual_in,
    gain_pre,
    gate_pre,
    up_pre,
    down_pre,
    gain_mix,
    query_weight,
    forget_weight,
    value_weight,
    outgate_weight,
    lower_bound,
    head_gain,
    out_weight,
    gain_post,
    gate_post,
    up_post,
    down_post,
    memory_state,
):
    nz, ny, tp = lax.axis_size("z"), lax.axis_size("y"), lax.axis_size(TP)
    z_at, t_at, y_at = (lax.axis_index(k).astype(jnp.uint32) for k in ("z", TP, "y"))
    own, width = residual_in.shape
    rows = nz * own
    units = gate_pre.shape[1]
    unit = -(-units * ny // (8 * tp)) * 8 * tp // ny
    block = width * tp // nz
    piece = block // tp
    halves = width // block
    kept = query_weight.shape[0]

    spread, stack, small = staged(
        unit,
        nz,
        z_at.astype(jnp.int32)[None],
        [residual_in, gate_pre.T, up_pre.T],
        [down_pre, gate_post.T, up_post.T, down_post],
        [query_weight, forget_weight, value_weight, outgate_weight],
        [v.reshape(-1, HEAD_DIM) for v in (gain_pre, gain_post, head_gain)],
        lower_bound.reshape(-1, HEAD_DIM),
        gain_mix.reshape(-1, block),
    )
    wide = width // HEAD_DIM
    own_first = stack[: 3 * unit]
    stack_1 = from_later(stack, "y", 1)
    first_2 = from_later(own_first, "y", 2)
    first_3 = from_later(own_first, "y", 3)
    first = [own_first, stack_1[: 3 * unit], first_2, first_3]
    middle = [*range(nz // 2, nz), *range(nz // 2)]
    all_rows = exchanged(spread, "z", [middle])
    all_rows = jnp.concatenate([all_rows[nz // 2 :], all_rows[: nz // 2]])
    gate_pre_t = jnp.concatenate([part[:unit] for part in first])
    up_pre_t = jnp.concatenate([part[unit : 2 * unit] for part in first])
    down_tiles = [part[2 * unit :].T.reshape(halves, tp, piece, unit) for part in first]
    down_tiles = jnp.stack(down_tiles).transpose(2, 0, 1, 3, 4)
    down_tiles = down_tiles.reshape(tp, ny * halves * piece, unit)
    mine = z_at // halves == t_at
    elsewhere = (jnp.arange(nz, dtype=jnp.uint32) // halves != t_at)[:, None]
    note_at = t_at * halves
    odd, upper = y_at % 2 == 1, y_at // 2 == 1
    second = jnp.concatenate([stack[3 * unit :], stack_1[3 * unit :]])
    gain_block = jnp.broadcast_to(small[6 * wide][:, None], (block, rows))
    all_rows, second, gate_pre_t, up_pre_t, down_tiles, *known = lax.optimization_barrier(
        (all_rows, second, gate_pre_t, up_pre_t, down_tiles, gain_block)
        + (mine, elsewhere, note_at, odd, upper, z_at)
        + tuple(small[k * wide : (k + 1) * wide] for k in range(6))
    )
    gain_block, mine, elsewhere, note_at, odd, upper, z_at = known[:7]
    gain_pre, gain_post, head_gain, log_floor, log_rest, rest_rate = known[7:]
    gain_pre, gain_post = gain_pre.reshape(width), gain_post.reshape(width)

    all_rows = all_rows.reshape(rows, width)
    turned = all_rows.T.reshape(halves, tp, piece, rows).swapaxes(0, 1)
    own_rows = (tp, halves * piece, rows)

    def finish(extra):
        pieces = extra[:, : halves * piece].reshape(nz, piece, rows)
        return (
            lax.dynamic_index_in_dim(pieces, z_at, axis=0, keepdims=False),
            *[extra[:, k * halves * piece :][:, : halves * piece].reshape(width, unit) for k in range(1, ny + 1)],
        )

    hidden, (residual, *down_pre_t, gain_block) = hidden_units(
        all_rows,
        gain_pre,
        gate_pre_t,
        up_pre_t,
        (turned.reshape(own_rows), down_tiles),
        finish,
        (gain_block,),
    )
    part = sum(
        dot(down_pre_t[k], hidden[k * unit : (k + 1) * unit], 1, 0) for k in range(ny)
    ).astype(bf16)
    part, residual, gain_block = lax.optimization_barrier((part, residual, gain_block))
    others = from_later(second, "y", 2)
    branch = exchanged(part.reshape(nz, piece, rows), "z")
    branch = branch.astype(f32).sum(axis=0)
    stream_piece = (residual.astype(f32) + 0.5 * branch).astype(bf16)

    second, others = lax.optimization_barrier((second, others))
    each = [part for pair in (second, others) for part in jnp.split(pair, 2)]
    gate_post_t, up_post_t, down_post_all = (
        jnp.concatenate([part[k * unit : (k + 1) * unit] for part in each]) for k in range(3)
    )
    mixers = jnp.concatenate(
        [
            jnp.concatenate([part[3 * unit + k * kept :][:kept] for part in each])
            for k in range(4)
        ],
        axis=1,
    )
    stream_piece, gate_post_t, up_post_t, down_post_all, mixers = lax.optimization_barrier(
        (stream_piece, gate_post_t, up_post_t, down_post_all, mixers)
    )
    stream_t = gathered(stream_piece, TP).reshape(block, rows)
    widened = stream_t.astype(f32)
    squares = jnp.sum(widened * widened, axis=0)
    scaled = reordered((widened * gain_block).astype(bf16), odd, upper)
    heads = width // HEAD_DIM
    parts = dot(scaled, mixers, 0, 0).astype(bf16)
    parts = parts.reshape(nz, own, 4 * heads, HEAD_DIM).swapaxes(1, 2)
    note = jnp.where(
        mine,
        stream_t.T.reshape(nz, own, block),
        jnp.broadcast_to(squares.astype(bf16).reshape(nz, own, 1), (nz, own, block)),
    )
    message = jnp.concatenate([parts.reshape(nz, 4 * heads * own, HEAD_DIM), note], axis=1)
    arrived = exchanged(message, "z")
    projected = arrived[:, : 4 * heads * own].astype(f32).sum(axis=0)
    notes = arrived[:, 4 * heads * own :]
    stream_a = lax.dynamic_slice_in_dim(notes, note_at, halves, axis=0)
    stream_a = stream_a.swapaxes(0, 1).reshape(own, width).astype(f32)
    total = jnp.sum(jnp.where(elsewhere, notes[:, :, 0].astype(f32), 0.0), axis=0)
    total = total + jnp.sum(stream_a * stream_a, axis=1)
    projected = projected.reshape(4, heads, own, HEAD_DIM)
    projected = projected * lax.rsqrt(total / D + EPSILON)[:, None]

    query_pre, forget_pre, value_pre, outgate_pre = (
        projected[k].swapaxes(0, 1) for k in range(4)
    )
    log_keep = jnp.logaddexp(log_floor, log_rest + jax.nn.log_sigmoid(forget_pre))
    inject = rest_rate * jax.nn.sigmoid(-forget_pre)
    next_state = (
        jnp.exp(log_keep)[..., None] * memory_state + inject[..., None] * value_pre[:, :, None, :]
    )
    readout = jnp.einsum(
        "bhk,bhkv->bhv", jax.nn.silu(query_pre), next_state, precision=lax.Precision.HIGHEST
    )
    normed = (
        readout
        * lax.rsqrt(jnp.mean(readout * readout, axis=2, keepdims=True) + EPSILON)
        * head_gain.reshape(heads, HEAD_DIM)
    )
    mixed_heads = (normed * jax.nn.silu(outgate_pre)).reshape(own, width).astype(bf16)
    partial_out = dot(mixed_heads, out_weight, 1, 0).astype(bf16)
    mixed = exchanged(partial_out.reshape(own, tp, width).swapaxes(0, 1), TP)
    stream_b = (stream_a + mixed.astype(f32).sum(axis=0)).astype(bf16)

    all_rows = gathered(stream_b, "z").reshape(rows, width)
    hidden, _ = hidden_units(all_rows, gain_post, gate_post_t, up_post_t, (), lambda _: (), ())
    part = dot(hidden, down_post_all, 0, 0).astype(bf16)
    branch = exchanged(part.reshape(nz, own, width), "z").astype(f32).sum(axis=0)
    layer_out = (stream_b.astype(f32) + 0.5 * branch).astype(bf16)
    return (layer_out, next_state)


def solution(mesh):
    grid = Mesh(mesh.devices.reshape(16, 4, 4, 2), ("z", "y", "x", "c"))
    kv = ("z", "y")
    in_specs = (
        P(kv, TP),
        P(TP),
        P(TP, kv),
        P(TP, kv),
        P(kv, TP),
        P(),
        P(kv, TP),
        P(kv, TP),
        P(kv, TP),
        P(kv, TP),
        P(TP),
        P(TP),
        P(TP, None),
        P(TP),
        P(TP, kv),
        P(TP, kv),
        P(kv, TP),
        P(kv, TP, None, None),
    )
    out_specs = (P(kv, TP), P(kv, TP, None, None))

    return jax.shard_map(shards, mesh=grid, in_specs=in_specs, out_specs=out_specs, check_vma=False)
```
